32 devices in a mesh: sp: 8 (over z, y), tp: 4 (over x, core).
Axes of the slice: x: 2, y: 2, z: 4, core: 2. Of those that a mesh axis runs over, the one named last changes fastest.
Arguments:
- skip_trunk_vector: bfloat16 [4096, 2048], P('sp', 'tp'), may hold values from -16 to 16
- valve_preactivation: bfloat16 [4096, 2048], P('sp', 'tp'), may hold values from -6 to 6
- projected_heads_payload: bfloat16 [4096, 2048], P('sp', 'tp'), may hold values from -6 to 6
- cluster_ingests: bfloat16 [4096, 1024], P('sp', 'tp'), may hold values from -6 to 6
- cluster_observers: bfloat16 [4096, 1024], P('sp', 'tp'), may hold values from -6 to 6
- pre_softplus_increments: float32 [2, 4096, 32], P(None, 'sp', 'tp'), may hold values from -6 to 6
- attenuation_ln_rate: float32 [2, 32], P(None, 'tp'), may hold values from -13 to -3
- additional_attenuation: float32 [2, 4096, 32], P(None, 'sp', 'tp'), may hold values from -3 to 0
- payload_conv_weights: float32 [7, 2048], P(None, 'tp'), may hold values from -2 to 2
- ingest_conv_weights: float32 [7, 1024], P(None, 'tp'), may hold values from -2 to 2
- observer_conv_weights: float32 [7, 1024], P(None, 'tp'), may hold values from -2 to 2
- valved_cluster_factor: float32 [2048], P('tp'), may hold values from 0.1 to 1.9
- closing_map_matrix: bfloat16 [2048, 2048], P('tp'), may hold values from -0.125 to 0.125
- dense_standardize_factor: float32 [2048], replicated, may hold values from 0.1 to 1.9
- dense_valve_map: bfloat16 [2048, 5120], P('sp', 'tp'), may hold values from -0.125 to 0.125
- dense_payload_map: bfloat16 [2048, 5120], P('sp', 'tp'), may hold values from -0.125 to 0.125
- valve_series_smoother: float32 [3, 5120], P(None, 'tp'), may hold values from -3.5 to 3.5
- payload_series_smoother: float32 [3, 5120], P(None, 'tp'), may hold values from -3.5 to 3.5
- dense_contract_map: bfloat16 [5120, 2048], P('tp', 'sp'), may hold values from -0.078125 to 0.078125
Outputs:
- updated: bfloat16 [4096, 2048], P('sp', 'tp')
The draws below stay inside these ranges and needn't reach their ends.
All inputs are finite; a program needn't handle non-finite values.
Results may differ from the reference program's by a relative error of at most 0.019.
Values may be sent and summed in bfloat16 or wider, within the bound.
A program may use at most 64 MiB of HBM per device.

```python
import jax
import jax.numpy as jnp
from jax import lax

TOK_DEV = 512
D = 2048
HEADS = 32
HEAD_DIM = 64
GROUPS = 8
STATE = 128
CONV = 7
FF = 5120
FF_TAPS = 3
MIXING_WIDTH = 2048
SEQUENCE_SPAN = 4096
N_TP = 4


def draw_skip_trunk_vector(key, part):
    column = jnp.arange(D, dtype=jnp.float32) / D
    scales = 0.5 * jnp.exp(jnp.log(5.0) * column)
    random_part = jax.random.truncated_normal(key, -6.0, 6.0, (SEQUENCE_SPAN, D), jnp.float32)
    return (random_part * scales).astype(jnp.bfloat16)


def draw_pre_softplus_increments(key, part):
    key_one, key_two = jax.random.split(key)
    blocks = SEQUENCE_SPAN // TOK_DEV
    offsets = jax.random.uniform(key_two, (2, blocks, 1, HEADS), jnp.float32, -1.2, 1.2)
    spread = jnp.broadcast_to(offsets, (2, blocks, TOK_DEV, HEADS)).reshape(2, SEQUENCE_SPAN, HEADS)
    random_part = jax.random.truncated_normal(key_one, -4.0, 4.0, (2, SEQUENCE_SPAN, HEADS), jnp.float32)
    return random_part + spread


def draw_attenuation_ln_rate(key, part):
    key_one, key_two, key_three = jax.random.split(key, 3)
    quick = jax.random.bernoulli(key_one, 0.5, (2, HEADS))
    slow_rate = jax.random.uniform(key_two, (2, HEADS), jnp.float32, 0.5, 1.0) * (0.6 / SEQUENCE_SPAN)
    fast_rate = jnp.exp(jax.random.uniform(key_three, (2, HEADS), jnp.float32, jnp.log(1.0 / 60.0), jnp.log(1.0 / 25.0)))
    return jnp.log(jnp.where(quick, fast_rate, slow_rate))


def draw_additional_attenuation(key, part):
    key_one, key_two = jax.random.split(key)
    places = jax.random.randint(key_one, (2, 4), 0, SEQUENCE_SPAN)
    kept_share = jax.random.uniform(key_two, (2, 4, HEADS), jnp.float32, 0.5, 0.8)
    position = jnp.arange(SEQUENCE_SPAN, dtype=jnp.int32)
    matches = (position[None, :, None] == places[:, None, :]).astype(jnp.float32)
    return jnp.einsum('dtk,dkh->dth', matches, jnp.log(kept_share))


def level_of(stream_key, extent, cuts, low, top_value):
    def one(axis_at, parts):
        heights = jax.random.uniform(jax.random.fold_in(jax.random.fold_in(stream_key, 6), axis_at), (parts,), jnp.float32, low / len(cuts), top_value / len(cuts))
        return jnp.repeat(jnp.exp(heights), extent[axis_at] // parts).reshape((-1,) + (1,) * (len(extent) - axis_at - 1))

    level = one(*cuts[0])
    for cut in cuts[1:]:
        level = level * one(*cut)
    return level


def noise(stream_key, extent, width, limit, cuts=(), held_as=jnp.bfloat16):
    factor_of = level_of(stream_key, extent, cuts, -0.22, 0.18) if cuts else 1.0
    array = jax.random.normal(stream_key, extent, jnp.float32) * width * factor_of
    return jnp.minimum(jnp.maximum(array, -limit), limit).astype(held_as)


def setup_inputs(seed: int = 0) -> dict:
    splits = jax.random.split(jax.random.key(seed), 20)
    return {
        "skip_trunk_vector": draw_skip_trunk_vector(jax.random.fold_in(splits[19], 71), 0),
        "valve_preactivation": noise(splits[1], (SEQUENCE_SPAN, MIXING_WIDTH), 1.0, 6.0, ((0, 8), (1, 4))),
        "projected_heads_payload": noise(splits[2], (SEQUENCE_SPAN, MIXING_WIDTH), 1.0, 6.0, ((0, 8), (1, 4))),
        "cluster_ingests": noise(splits[3], (SEQUENCE_SPAN, GROUPS * STATE), 1.0, 6.0, ((0, 8), (1, 4))),
        "cluster_observers": noise(splits[4], (SEQUENCE_SPAN, GROUPS * STATE), 1.0, 6.0, ((0, 8), (1, 4))),
        "pre_softplus_increments": draw_pre_softplus_increments(jax.random.fold_in(splits[19], 71), 0),
        "attenuation_ln_rate": draw_attenuation_ln_rate(jax.random.fold_in(splits[19], 71), 0),
        "additional_attenuation": draw_additional_attenuation(jax.random.fold_in(splits[19], 71), 0),
        "payload_conv_weights": noise(splits[8], (CONV, MIXING_WIDTH), CONV ** -0.5, 2.0, ((1, 4),), jnp.float32),
        "ingest_conv_weights": noise(splits[9], (CONV, GROUPS * STATE), CONV ** -0.5, 2.0, ((1, 4),), jnp.float32),
        "observer_conv_weights": noise(splits[10], (CONV, GROUPS * STATE), CONV ** -0.5, 2.0, ((1, 4),), jnp.float32),
        "valved_cluster_factor": jnp.clip(1.0 + 0.18 * jax.random.normal(splits[11], (MIXING_WIDTH,), jnp.float32), 0.1, 1.9),
        "closing_map_matrix": noise(splits[12], (MIXING_WIDTH, D), MIXING_WIDTH ** -0.5, 0.125, ((0, 4),)),
        "dense_standardize_factor": jnp.clip(1.0 + 0.18 * jax.random.normal(splits[13], (D,), jnp.float32), 0.1, 1.9),
        "dense_valve_map": noise(splits[14], (D, FF), D ** -0.5, 0.125, ((0, 8), (1, 4))),
        "dense_payload_map": noise(splits[15], (D, FF), D ** -0.5, 0.125, ((0, 8), (1, 4))),
        "valve_series_smoother": noise(splits[16], (FF_TAPS, FF), FF_TAPS ** -0.5, 3.5, ((1, 4),), jnp.float32),
        "payload_series_smoother": noise(splits[17], (FF_TAPS, FF), FF_TAPS ** -0.5, 3.5, ((1, 4),), jnp.float32),
        "dense_contract_map": noise(splits[18], (FF, D), FF ** -0.5, 0.078125, ((0, 4), (1, 8))),
    }


EPSILON = 1e-06

def centred_conv(data, kernel):
    margin = kernel.shape[0] // 2
    length = data.shape[0]
    padded = jnp.pad(data, ((margin, margin), (0, 0)))
    summed = padded[0:length] * kernel[0]
    for offset in range(1, kernel.shape[0]):
        summed = summed + padded[offset:offset + length] * kernel[offset]
    return summed

def one_way(values_f, inputs_h, readout_h, stride_lengths_change, fading_exponent):
    blocks = SEQUENCE_SPAN // TOK_DEV
    places = jnp.arange(TOK_DEV, dtype=jnp.int32)
    lower_mask = places[:, None] >= places[None, :]

    def advance(carried, pieces):
        block_values, block_inputs, block_readout, block_steps, block_logs = pieces
        running = jnp.cumsum(block_logs, axis=0)
        log_gaps = running.T[:, :, None] - running.T[:, None, :]
        decays = jnp.exp(jnp.where(lower_mask[None], log_gaps, -jnp.inf))
        scores = jnp.einsum('thn,shn->hts', block_readout, block_inputs, precision=lax.Precision.HIGHEST)
        weights = scores * decays * block_steps.T[:, None, :]
        within = jnp.einsum('hts,shp->thp', weights, block_values, precision=lax.Precision.HIGHEST)
        outer = jnp.einsum('thn,hpn->thp', block_readout, carried, precision=lax.Precision.HIGHEST)
        outer = outer * jnp.exp(running)[:, :, None]
        to_end = jnp.exp(running[-1][None, :] - running) * block_steps
        block_state = jnp.einsum('sh,shp,shn->hpn', to_end, block_values, block_inputs, precision=lax.Precision.HIGHEST)
        carried = carried * jnp.exp(running[-1])[:, None, None] + block_state
        return (carried, within + outer)
    pieces = (values_f.reshape(blocks, TOK_DEV, HEADS, HEAD_DIM), inputs_h.reshape(blocks, TOK_DEV, HEADS, STATE), readout_h.reshape(blocks, TOK_DEV, HEADS, STATE), stride_lengths_change.reshape(blocks, TOK_DEV, HEADS), fading_exponent.reshape(blocks, TOK_DEV, HEADS))
    start_state = jnp.zeros((HEADS, HEAD_DIM, STATE), jnp.float32)
    final_state, results = lax.scan(advance, start_state, pieces)
    return results.reshape(SEQUENCE_SPAN, HEADS, HEAD_DIM)

def split_product(left, right, part_width, out_width):

    def add_part(summed, index):
        start = index * part_width
        columns = lax.dynamic_slice_in_dim(left, start, part_width, 1)
        rows_part = lax.dynamic_slice_in_dim(right, start, part_width, 0)
        term = jnp.dot(columns, rows_part, preferred_element_type=jnp.float32).astype(jnp.bfloat16)
        return (summed + lax.optimization_barrier(term).astype(jnp.float32), index)
    zero_sum = jnp.zeros((left.shape[0], out_width), jnp.float32)
    summed, indices = lax.scan(add_part, zero_sum, jnp.arange(N_TP, dtype=jnp.int32))
    return summed

def reference(skip_trunk_vector, valve_preactivation, projected_heads_payload, cluster_ingests, cluster_observers, pre_softplus_increments, attenuation_ln_rate, additional_attenuation, payload_conv_weights, ingest_conv_weights, observer_conv_weights, valved_cluster_factor, closing_map_matrix, dense_standardize_factor, dense_valve_map, dense_payload_map, valve_series_smoother, payload_series_smoother, dense_contract_map):
    per_group = HEADS // GROUPS
    mixed_values = jax.nn.silu(centred_conv(projected_heads_payload.astype(jnp.float32), payload_conv_weights)).astype(jnp.bfloat16)
    mixed_inputs = jax.nn.silu(centred_conv(cluster_ingests.astype(jnp.float32), ingest_conv_weights)).astype(jnp.bfloat16)
    mixed_readout = jax.nn.silu(centred_conv(cluster_observers.astype(jnp.float32), observer_conv_weights)).astype(jnp.bfloat16)
    values_f = mixed_values.astype(jnp.float32).reshape(SEQUENCE_SPAN, HEADS, HEAD_DIM)
    inputs_h = jnp.repeat(mixed_inputs.astype(jnp.float32).reshape(SEQUENCE_SPAN, GROUPS, STATE), per_group, axis=1)
    readout_h = jnp.repeat(mixed_readout.astype(jnp.float32).reshape(SEQUENCE_SPAN, GROUPS, STATE), per_group, axis=1)
    stride_lengths_change = jax.nn.softplus(pre_softplus_increments)
    fading_exponent = additional_attenuation - stride_lengths_change * jnp.exp(attenuation_ln_rate)[:, None, :]
    forward = one_way(values_f, inputs_h, readout_h, stride_lengths_change[0], fading_exponent[0])
    backward = jnp.flip(one_way(jnp.flip(values_f, 0), jnp.flip(inputs_h, 0), jnp.flip(readout_h, 0), jnp.flip(stride_lengths_change[1], 0), jnp.flip(fading_exponent[1], 0)), 0)
    gated = (forward + backward).reshape(SEQUENCE_SPAN, MIXING_WIDTH) * jax.nn.silu(valve_preactivation.astype(jnp.float32))
    grouped = gated.reshape(SEQUENCE_SPAN, GROUPS, MIXING_WIDTH // GROUPS)
    standardized = grouped * lax.rsqrt(lax.optimization_barrier(jnp.mean(grouped * grouped, axis=2, keepdims=True)) + EPSILON)
    blending_result = (standardized.reshape(SEQUENCE_SPAN, MIXING_WIDTH) * valved_cluster_factor).astype(jnp.bfloat16)
    mapped_vector = split_product(blending_result, closing_map_matrix, MIXING_WIDTH // N_TP, D)
    intermediate_hidden = (skip_trunk_vector.astype(jnp.float32) + mapped_vector).astype(jnp.bfloat16)
    middle_f = intermediate_hidden.astype(jnp.float32)
    scaled = middle_f * lax.rsqrt(lax.optimization_barrier(jnp.mean(middle_f * middle_f, axis=1, keepdims=True)) + EPSILON)
    normed_rows = (scaled * dense_standardize_factor).astype(jnp.bfloat16)
    gate_rows = jnp.dot(normed_rows, dense_valve_map, preferred_element_type=jnp.float32).astype(jnp.bfloat16)
    value_rows = jnp.dot(normed_rows, dense_payload_map, preferred_element_type=jnp.float32).astype(jnp.bfloat16)
    gate_conv = centred_conv(gate_rows.astype(jnp.float32), valve_series_smoother)
    value_conv = centred_conv(value_rows.astype(jnp.float32), payload_series_smoother)
    hidden = (jax.nn.silu(gate_conv) * value_conv).astype(jnp.bfloat16)
    down_sum = split_product(hidden, dense_contract_map, FF // N_TP, D)
    return (middle_f + down_sum).astype(jnp.bfloat16)
```

```python
import math

import jax
import jax.numpy as jnp
from jax import lax
from jax.sharding import Mesh
from jax.sharding import PartitionSpec as P

HEADS = 32
GROUPS = 8
STATE = 128
EPSILON = 1e-06
SP = ("z", "y")
TP = ("x", "core")


def shifted(block, axis, step):
    count = lax.axis_size(axis)
    return lax.ppermute(block, axis, [(i, (i + step) % count) for i in range(count)])


def moved(block, axis, step):
    count = lax.axis_size(axis)
    pairs = [(i, i + step) for i in range(count) if 0 <= i + step < count]
    return lax.ppermute(block, axis, pairs)


def grid_shifted(block, axes, steps):
    sizes = [lax.axis_size(a) for a in axes]
    pairs = []
    for source in range(sizes[0] * sizes[1]):
        first, second = divmod(source, sizes[1])
        target = ((first + steps[0]) % sizes[0]) * sizes[1] + (second + steps[1]) % sizes[1]
        pairs.append((source, target))
    return lax.ppermute(block, axes, pairs)


def ordered(by_step, index):
    count = len(by_step)
    result = []
    for owner in range(count):
        back = lax.rem(index - owner + count, count)
        block = by_step[0]
        for step in range(1, count):
            block = jnp.where(back == step, by_step[step], block)
        result.append(block)
    return result


def extended(block, axis, width):
    low = moved(block[-width:], axis, 1)
    high = moved(block[:width], axis, -1)
    return jnp.concatenate([low, block, high], axis=0)


def conv_rows(padded, kernel, length):
    summed = padded[0:length] * kernel[0]
    for offset in range(1, kernel.shape[0]):
        summed = summed + padded[offset : offset + length] * kernel[offset]
    return summed


def bdot(pattern, one, two):
    return jnp.einsum(pattern, one, two, preferred_element_type=jnp.float32)


def pack(decay, state):
    heads, width, depth = state.shape
    rows = jnp.broadcast_to(decay[:, None, None], (heads, 16, depth)).astype(jnp.bfloat16)
    return jnp.concatenate([state.astype(jnp.bfloat16), rows], axis=1)


def unpack(packed, width):
    body = packed.astype(jnp.float32)
    return body[:, width, 0], body[:, :width]


def carried_in(decay, state, sign):
    width = state.shape[1]
    count = lax.axis_size(SP)
    own = pack(decay, state)
    index = lax.axis_index(SP)

    def from_back(array, step):
        back, value = unpack(moved(array, SP, sign * step), width)
        source = index - sign * step
        inside = (source >= 0) & (source < count)
        return jnp.where(inside, back, 1.0), value

    near, far = from_back(own, 1), from_back(own, 2)
    total = near[1] + near[0][:, None, None] * far[1]
    product = near[0] * far[0]
    covered = 2
    while covered < count - 1:
        back, value = from_back(pack(product, total), covered)
        total = total + product[:, None, None] * value
        product = product * back
        covered *= 2
    return total


def tied(value, *others):
    marks = [other[(slice(0, 1),) * other.ndim] for other in others]
    return lax.optimization_barrier((value, *marks))[0]


def shared_rows(weight, axis_dim, out_dim, mark):
    count = lax.axis_size("y")
    index = lax.axis_index("y")
    part = weight.shape[axis_dim] // count
    received = []
    for step in range(count):
        at = lax.rem(index + step, count) * part
        block = lax.dynamic_slice_in_dim(weight, at, part, axis_dim)
        received.append(shifted(block, "y", step) if step else block)
    received = [tied(block, mark) for block in received]
    return jnp.concatenate(ordered(received, index), axis=out_dim)


def shards(
    skip_trunk_vector,
    valve_preactivation,
    projected_heads_payload,
    cluster_ingests,
    cluster_observers,
    pre_softplus_increments,
    attenuation_ln_rate,
    additional_attenuation,
    payload_conv_weights,
    ingest_conv_weights,
    observer_conv_weights,
    valved_cluster_factor,
    closing_map_matrix,
    dense_standardize_factor,
    dense_valve_map,
    dense_payload_map,
    valve_series_smoother,
    payload_series_smoother,
    dense_contract_map,
):
    rows = skip_trunk_vector.shape[0]
    own_cols = skip_trunk_vector.shape[1]
    head_count = pre_softplus_increments.shape[2]
    per_group = HEADS // GROUPS
    nx, nc, ny = lax.axis_size("x"), lax.axis_size("core"), lax.axis_size("y")
    ix, ic, iy = lax.axis_index("x"), lax.axis_index("core"), lax.axis_index("y")

    joined = jnp.concatenate([projected_heads_payload, cluster_ingests, cluster_observers], axis=1)
    taps_all = jnp.concatenate(
        [payload_conv_weights, ingest_conv_weights, observer_conv_weights], axis=1
    )
    padded = extended(joined, SP, taps_all.shape[0] // 2)

    convolved = jax.nn.silu(conv_rows(padded.astype(jnp.float32), taps_all, rows)).astype(
        jnp.bfloat16
    )
    gate_w = lax.all_gather(shared_rows(dense_valve_map, 1, 0, convolved), "z", axis=0, tiled=True)
    value_w = lax.all_gather(
        shared_rows(dense_payload_map, 1, 0, convolved), "z", axis=0, tiled=True
    )

    payload_columns = projected_heads_payload.shape[1]
    input_cols = cluster_ingests.shape[1]
    width = payload_columns // head_count
    groups = input_cols // STATE
    values = convolved[:, :payload_columns]
    inputs_g = convolved[:, payload_columns : payload_columns + input_cols].reshape(
        rows, groups, STATE
    )
    readout_g = convolved[:, payload_columns + input_cols :].reshape(rows, groups, STATE)

    steps = jax.nn.softplus(pre_softplus_increments)
    logs = additional_attenuation - steps * jnp.exp(attenuation_ln_rate)[:, None, :]
    running = jnp.cumsum(logs, axis=1)
    run_f = running[0]
    exc_b = running[1] - logs[1]
    total_f, total_b = running[0, -1], running[1, -1]

    end_f = jnp.exp(total_f[None] - run_f) * steps[0]
    end_b = jnp.exp(exc_b) * steps[1]
    ends = jnp.stack([end_f, end_b], axis=1)
    scaled = (
        ends[:, :, :, None] * values.astype(jnp.float32).reshape(rows, 1, head_count, width)
    ).astype(jnp.bfloat16)
    scaled = scaled.reshape(rows, 2, groups, per_group, width)
    summary = bdot("sdgep,sgn->dgepn", scaled, inputs_g).reshape(2, head_count, width, STATE)
    in_f = carried_in(jnp.exp(total_f), summary[0], 1)
    in_b = carried_in(jnp.exp(total_b), summary[1], -1)

    down_part = shared_rows(dense_contract_map, 0, 1, in_f)
    down_w = lax.all_gather(down_part, "z", axis=1, tiled=True)

    places = jnp.arange(rows, dtype=jnp.int32)
    after = places[:, None] > places[None, :]
    same = places[:, None] == places[None, :]
    run_fT, exc_bT = run_f.T, exc_b.T
    step_f, step_b = steps[0].T, steps[1].T
    gaps = jnp.where(
        after[None],
        run_fT[:, :, None] - run_fT[:, None, :],
        exc_bT[:, None, :] - exc_bT[:, :, None],
    )
    factor = jnp.where(
        after[None],
        step_f[:, None, :],
        jnp.where(same[None], (step_f + step_b)[:, None, :], step_b[:, None, :]),
    )
    scores = jnp.repeat(bdot("tgn,sgn->gts", readout_g, inputs_g), per_group, axis=0)
    weights = (scores * jnp.exp(gaps) * factor).astype(jnp.bfloat16)
    within = bdot("hts,shp->thp", weights, values.reshape(rows, head_count, width))

    def outer(state):
        grouped = state.astype(jnp.bfloat16).reshape(groups, per_group, width, STATE)
        return bdot("gepn,tgn->tgep", grouped, readout_g).reshape(rows, head_count, width)

    mixed = within + outer(in_f) * jnp.exp(run_f)[:, :, None]
    mixed = mixed + outer(in_b) * jnp.exp(total_b[None] - exc_b)[:, :, None]
    gated = mixed.reshape(rows, payload_columns) * jax.nn.silu(
        valve_preactivation.astype(jnp.float32)
    )
    grouped = gated.reshape(rows, groups, per_group * width)
    standardized = grouped * lax.rsqrt(jnp.mean(grouped * grouped, axis=2, keepdims=True) + EPSILON)
    blended = (standardized.reshape(rows, payload_columns) * valved_cluster_factor).astype(
        jnp.bfloat16
    )

    def column_block(matrix, dx, dc):
        at = (lax.rem(ix + dx, nx) * nc + lax.rem(ic + dc, nc)) * own_cols
        return lax.dynamic_slice_in_dim(matrix, at, own_cols, 1)

    def over_cores(terms):
        total = terms[0].astype(jnp.bfloat16).astype(jnp.float32)
        for dc in range(1, nc):
            total = total + shifted(terms[dc].astype(jnp.bfloat16), "core", dc).astype(jnp.float32)
        return total

    mapped = None
    for dx in list(range(1, nx)) + [0]:
        terms = [
            jnp.dot(
                blended,
                column_block(closing_map_matrix, dx, dc),
                preferred_element_type=jnp.float32,
            )
            for dc in range(nc)
        ]
        part = over_cores(terms)
        if dx:
            part = shifted(part.astype(jnp.bfloat16), "x", dx).astype(jnp.float32)
        mapped = part if mapped is None else mapped + part
    middle = (skip_trunk_vector.astype(jnp.float32) + mapped).astype(jnp.bfloat16)

    margin = valve_series_smoother.shape[0] // 2
    room = -(-margin // 16) * 16
    low = moved(middle[-margin:], SP, 1)
    high = moved(middle[:margin], SP, -1)
    blank = jnp.zeros((room - margin, own_cols), middle.dtype)
    wide = jnp.concatenate([blank, low, middle, high, blank], axis=0)

    def everywhere(block):
        by_y = []
        for dy in range(ny):
            by_x = []
            for dx in range(nx):
                got = grid_shifted(block, ("y", "x"), (dy, dx)) if dy or dx else block
                by_core = [got] + [shifted(got, "core", dc) for dc in range(1, nc)]
                by_x.append(jnp.concatenate(ordered(by_core, ic), axis=1))
            by_y.append(jnp.concatenate(ordered(by_x, ix), axis=1))
        return jnp.stack(ordered(by_y, iy))

    line = everywhere(wide).reshape(ny * (rows + 2 * room), -1).astype(jnp.float32)
    inverse = lax.rsqrt(jnp.mean(line * line, axis=1, keepdims=True) + EPSILON)
    normed = (line * inverse * dense_standardize_factor).astype(jnp.bfloat16)

    hidden_cols = gate_w.shape[1]
    gate_taps = lax.dynamic_slice_in_dim(valve_series_smoother, iy * hidden_cols, hidden_cols, 1)
    value_taps = lax.dynamic_slice_in_dim(payload_series_smoother, iy * hidden_cols, hidden_cols, 1)

    def spread(weight, taps):
        made = jnp.dot(normed, weight, preferred_element_type=jnp.float32).astype(jnp.bfloat16)
        made = made.reshape(ny, rows + 2 * room, hidden_cols).astype(jnp.float32)
        summed = None
        for offset in range(taps.shape[0]):
            start = room - margin + offset
            term = made[:, start : start + rows] * taps[offset]
            summed = term if summed is None else summed + term
        return summed

    gate_rows = spread(gate_w, gate_taps)
    value_rows = spread(value_w, value_taps)
    hidden = (jax.nn.silu(gate_rows) * value_rows).astype(jnp.bfloat16)

    order = [(dy, dx) for dy in range(ny) for dx in range(nx)]
    down = None
    for dy, dx in order[1:] + order[:1]:
        wanted = lax.dynamic_index_in_dim(hidden, lax.rem(iy + dy, ny), 0, keepdims=False)
        terms = [
            jnp.dot(wanted, column_block(down_w, dx, dc), preferred_element_type=jnp.float32)
            for dc in range(nc)
        ]
        part = over_cores(terms)
        if dy or dx:
            part = grid_shifted(part.astype(jnp.bfloat16), ("y", "x"), (dy, dx)).astype(jnp.float32)
        down = part if down is None else down + part
    return (middle.astype(jnp.float32) + down).astype(jnp.bfloat16)


def solution(mesh):
    sp, tp = mesh.shape["sp"], mesh.shape["tp"]
    ny = 2 ** (int(math.log2(sp)) // 2)
    nc = 2 if tp % 2 == 0 else 1
    grid = Mesh(
        mesh.devices.reshape(sp // ny, ny, tp // nc, nc), ("z", "y", "x", "core")
    )
    return jax.shard_map(
        shards,
        mesh=grid,
        in_specs=(
            P(SP, TP),
            P(SP, TP),
            P(SP, TP),
            P(SP, TP),
            P(SP, TP),
            P(None, SP, TP),
            P(None, TP),
            P(None, SP, TP),
            P(None, TP),
            P(None, TP),
            P(None, TP),
            P(TP),
            P(TP, None),
            P(),
            P(SP, TP),
            P(SP, TP),
            P(None, TP),
            P(None, TP),
            P(TP, SP),
        ),
        out_specs=P(SP, TP),
        check_vma=False,
    )
```
